32 devices in a mesh: ep: 8 (over z, y), tp: 4 (over x, core).
Axes of the slice: x: 2, y: 2, z: 4, core: 2. Of those that a mesh axis runs over, the one named last changes fastest.
Arguments:
- tokens: bfloat16 [2048, 2048], P('ep', 'tp'), may hold values from -72 to 72
- norm_gain: bfloat16 [2048], P('tp'), may hold values from 0.099609375 to 1.8984375
- expert_ids: int32 [2048, 2], P('ep'), may hold values from 0 to 7, all different within a row; in each aligned block of 256 rows (0 to 255, 256 to 511, ...) at most 128 rows name the same one
- gate_share: float32 [2048, 2], P('ep'), may hold values from 0.1 to 1
- gate_weight: bfloat16 [8, 2048, 4096], P('ep', None, 'tp'), may hold values from -0.125 to 0.125
- up_weight: bfloat16 [8, 2048, 4096], P('ep', None, 'tp'), may hold values from -0.125 to 0.125
- down_weight: bfloat16 [8, 4096, 2048], P('ep', 'tp'), may hold values from -0.09375 to 0.09375
Outputs:
- mixed: bfloat16 [2048, 2048], P('ep', 'tp')
The draws below stay inside these ranges and needn't reach their ends.
Inputs may be any that keep to these rules, and one draw needn't show every extreme that they name: `expert_ids`: each token names two different experts; among the 256 tokens of one index of ep no expert is named more than 128 times, a bound that some block reaches.
All inputs are finite; a program needn't handle non-finite values.
Results may differ from the reference program's by a relative error of at most 0.019.
Values may be sent and summed in bfloat16 or wider, within the bound.
A program may use at most 64 MiB of HBM per device.

```python
import math
import jax
import jax.numpy as jnp
import numpy as np
from jax import lax

D = 2048
FF = 4096
TOK_DEV = 256
EXPERTS = 8
CAP = 128
TOKENS = 2048
N_EP = 8
N_TP = 4


def draw_tokens(key, part):
    first, second, third = jax.random.split(key, 3)
    scales = jnp.exp(jax.random.uniform(second, (N_TP,), jnp.float32, jnp.log(0.3), jnp.log(3.0)))
    columns = jnp.repeat(scales, D // N_TP)
    base = jnp.clip(jax.random.normal(first, (TOKENS, D), jnp.float32), -6.0, 6.0)
    return (base * columns[None, :]).astype(jnp.bfloat16)


def levels(rng, extent, pieces, smallest, high):
    def one(dim, shards_of):
        draws = jax.random.uniform(jax.random.fold_in(jax.random.fold_in(rng, 6), dim), (shards_of,), jnp.float32, smallest / len(pieces), high / len(pieces))
        return jnp.repeat(jnp.exp(draws), extent[dim] // shards_of).reshape((-1,) + (1,) * (len(extent) - dim - 1))

    factor_of = one(*pieces[0])
    for cut in pieces[1:]:
        factor_of = factor_of * one(*cut)
    return factor_of


def routed_block(own_key, own, number, rows, count, top, most, skew):
    ranking = jax.random.permutation(own_key, count)
    packed, common = portions_of(count, rows * top, most, skew, True), portions_of(count, rows * top, most, skew, False)
    places = jnp.arange(count)

    def named(lengths, turn):
        used = int((lengths > 0).sum())
        fixed = max(1, used // 4)
        passed = fixed + (places - fixed + turn * (used - fixed)) % max(1, count - fixed)
        return jnp.zeros((count,), jnp.int32).at[ranking[jnp.where(places < fixed, places, passed)]].set(jnp.asarray(lengths, jnp.int32))

    lengths = jnp.where(number % 4 == 0, named(packed, number // 4), named(common, number - number // 4 - 1))
    mixed = jax.random.permutation(jax.random.fold_in(own, 3), count)
    source_of, sink = mixed[0:count // 2 * 2:2], mixed[1:count // 2 * 2:2]
    slack = jnp.minimum(lengths[source_of] - 1, most - lengths[sink]) // 2
    slack = jnp.where((source_of == ranking[0]) | (sink == ranking[0]) | (lengths[sink] == 0), 0, jnp.maximum(slack, 0))
    passed = jax.random.randint(jax.random.fold_in(own, 4), (count // 2,), 0, 1 << 20) % (slack + 1)
    lengths = lengths.at[source_of].add(-passed).at[sink].add(passed)
    members = jnp.searchsorted(jnp.cumsum(lengths), jnp.arange(rows * top), side="right").astype(jnp.int32)
    table = members.reshape(top, rows).T
    table = table[jax.random.permutation(jax.random.fold_in(own, 1), rows)]
    turn = jax.random.randint(jax.random.fold_in(own, 2), (rows, 1), 0, top)
    return jnp.take_along_axis(table, (jnp.arange(top)[None, :] + turn) % top, axis=1)


def portions_of(count, total, limit, skew, full):
    loads = [(1 << 20) // math.isqrt(standing ** skew) + 1 for standing in range(1, count + 1)]
    largest = limit if full else min(limit, max(-(-total // count), total * loads[0] // sum(loads)))
    least = 1 if total - largest >= count - 1 else 0
    given, spare = [largest] + [least] * (count - 1), total - largest - least * (count - 1)
    while spare > 0:
        free = [i for i in range(1, count) if given[i] < largest] or [i for i in range(1, count) if given[i] < limit]
        mass, remaining = sum([loads[i] for i in free]), spare
        for i in free:
            addition = min(limit - given[i], max(1, remaining * loads[i] // mass), spare)
            given[i] = given[i] + addition
            spare = spare - addition
    return np.array(given)


def normal_values(own_key, shape, scale, most, shards=(), kind=jnp.bfloat16):
    result = scale * jax.random.normal(own_key, shape, jnp.float32)
    if shards:
        result = result * levels(own_key, shape, shards, -0.22, 0.18)
    return jnp.clip(result, -most, most).astype(kind)


def setup_inputs(seed: int = 0) -> dict:
    arg_keys = jax.random.split(jax.random.key(seed), 8)
    tokens = draw_tokens(jax.random.fold_in(arg_keys[7], 71), 0)
    norm_gain = jnp.clip(1.0 + 0.18 * jax.random.normal(arg_keys[1], (D,), jnp.float32), 0.099609375, 1.8984375).astype(jnp.bfloat16)
    expert_ids_keys = jax.random.split(jax.random.fold_in(arg_keys[2], 1), TOKENS // TOK_DEV)
    expert_ids_turns = jax.random.permutation(jax.random.fold_in(arg_keys[2], 3), TOKENS // TOK_DEV)
    expert_ids = jax.vmap(lambda own, number: routed_block(jax.random.fold_in(arg_keys[2], 2), own, number, TOK_DEV, EXPERTS, 2, CAP, 2))(expert_ids_keys, expert_ids_turns).reshape((TOKENS, 2))
    gate_share = jnp.clip(0.1 + 0.9 * jax.random.uniform(arg_keys[3], (TOKENS, 2), jnp.float32) ** levels(arg_keys[3], (TOKENS, 2), ((0, 8),), -0.2, 0.2), 0.1, 1.0)
    gate_weight = normal_values(arg_keys[4], (EXPERTS, D, FF), D ** -0.5, 0.125, ((0, 8), (2, 4)))
    up_weight = normal_values(arg_keys[5], (EXPERTS, D, FF), D ** -0.5, 0.125, ((0, 8), (2, 4)))
    down_weight = normal_values(arg_keys[6], (EXPERTS, FF, D), FF ** -0.5, 0.09375, ((0, 8), (1, 4)))
    return {"tokens": tokens, "norm_gain": norm_gain, "expert_ids": expert_ids, "gate_share": gate_share, "gate_weight": gate_weight, "up_weight": up_weight, "down_weight": down_weight}


EPS = 1e-06

def reference(tokens, norm_gain, expert_ids, gate_share, gate_weight, up_weight, down_weight):
    xf = tokens.astype(jnp.float32)
    factor = lax.rsqrt(lax.optimization_barrier(jnp.mean(xf * xf, axis=1, keepdims=True)) + EPS)
    normed = (xf * factor * norm_gain.astype(jnp.float32)[None, :]).astype(jnp.bfloat16)
    blocks = expert_ids.reshape(N_EP, TOK_DEV * 2)
    onehot = (blocks[:, :, None] == jnp.arange(EXPERTS, dtype=jnp.int32)[None, None, :]).astype(jnp.int32)
    slots = lax.optimization_barrier(jnp.sum((jnp.cumsum(onehot, axis=1) - onehot) * onehot, axis=2))
    source = jnp.arange(N_EP, dtype=jnp.int32)[:, None]
    position = (source * CAP + slots).reshape(-1).astype(jnp.int32)
    flat_ids = expert_ids.reshape(-1).astype(jnp.int32)
    rows = jnp.repeat(normed, 2, axis=0)
    buffer = jnp.zeros((EXPERTS, N_EP * CAP, D), jnp.bfloat16).at[flat_ids, position].set(rows)
    width = FF // N_TP

    def expert(args):
        buf, w_gate, w_up, w_down = args
        gate = jnp.dot(buf, w_gate, preferred_element_type=jnp.float32)
        upper = jnp.dot(buf, w_up, preferred_element_type=jnp.float32)
        hidden = (jax.nn.silu(gate) * upper).astype(jnp.bfloat16)

        def add_block(index, total):
            piece = lax.dynamic_slice_in_dim(hidden, index * width, width, 1)
            wpiece = lax.dynamic_slice_in_dim(w_down, index * width, width, 0)
            term = jnp.dot(piece, wpiece, preferred_element_type=jnp.float32).astype(jnp.bfloat16)
            return total + lax.optimization_barrier(term).astype(jnp.float32)
        total = lax.fori_loop(0, N_TP, add_block, jnp.zeros((buf.shape[0], D), jnp.float32))
        return total.astype(jnp.bfloat16)
    outputs = lax.map(expert, (buffer, gate_weight, up_weight, down_weight))
    picked = outputs[flat_ids, position].astype(jnp.float32).reshape(TOKENS, 2, D)
    return lax.optimization_barrier(jnp.sum(picked * gate_share[:, :, None], axis=1)).astype(jnp.bfloat16)
```

```python
import functools
import jax
import jax.numpy as jnp
from jax import lax
from jax.experimental import pallas as pl
from jax.experimental.pallas import tpu as pltpu
from jax.sharding import PartitionSpec as P

D = 2048


EPS = 1e-06
MESH = pl.DeviceIdType.MESH
BF = jnp.bfloat16
F32 = jnp.float32
CORES = 2
LINE = 2
mark = jax.named_scope
SENDS = (
    "6/2", "4/3", "2/1", "3/4", "1/6", "7/5", "5/7",
)
NEAR = 3
LAST = "5"
ORDER = (
    "take:0", "take:1", "pass:0", "<take:6",
    "load:0", "ready:0", "norm:0", "gu0:0", "gu1:0", "gu2:0", "gu3:0", "away:0", "here:0",
    ">take:6", "<take:2", "pass:1",
    "ready:1", "norm:1", "gu0:1", "gu1:1", "home:0", "<take:3", ">take:4", "gu2:1", "gu3:1",
    "<pass:6", ">take:2", "away:1", "here:1", ">pass:6",
    "ready:6", "norm:6", "gu0:6", "home:1", "gu1:6", ">take:3", "gu2:6", "gu3:6", "pass:2/4",
    "away:6", "<take:4", "here:6",
    "ready:2/4", "norm:2/4", "gu0:2/4", "pair:6", "gu1:2/4", "gu2:2/4", "gu3:2/4", "pass:3/2",
    "away:2/4", "take:7", "here:2/4",
    "ready:3/2", "norm:3/2", "gu0:3/2", "<home:2", ">pair:4", "gu1:3/2", ">take:5", "gu2:3/2",
    "gu3:3/2", ">pass:3", "<pass:4", "away:3/2", "here:3/2", "<take:5",
    "ready:4/3", "norm:4/3", "gu0:4/3", ">home:2", ">give:6", "gu1:4/3", "<give:6", "gu2:4/3",
    "gu3:4/3", "pass:7", "away:4/3", "here:4/3", "<pair:3",
    "ready:7", "norm:7", "gu0:7", "<pair:4", ">pair:3", "gu1:7", ">give:4", "gu2:7", "gu3:7",
    ">pass:5", "away:7", "here:7", "<pass:5",
    "ready:5", "norm:5", "gu0:5", "pair:7", "gu1:5", "gu2:5", "gu3:5", "away:5", "<give:4",
    "<give:3", "here:5",
    "collect:1", "collect:2", "pair:5", ">give:3", "give:7", "swap:0", "give:5", "gather:0",
    "mix:6", "mix:4", "mix:3", "mix:7",
)


def plain(tokens, norm_gain, expert_ids, gate_share, gate_weight, up_weight, down_weight):
    n_expdev = lax.axis_size("ep")
    exp_local = gate_weight.shape[0]
    experts = exp_local * n_expdev
    tok_rows = tokens.shape[0]
    slot_cap = 4 * tok_rows // experts
    flat_ids = expert_ids.reshape(-1)
    onehot = (flat_ids[:, None] == jnp.arange(experts, dtype=jnp.int32)[None, :]).astype(jnp.int32)
    slots = jnp.sum((jnp.cumsum(onehot, axis=0) - onehot) * onehot, axis=1)
    target = flat_ids * slot_cap + slots
    values = tokens.astype(jnp.float32)
    squares = lax.psum(jnp.sum(values * values, axis=1), "tp")
    factor = lax.rsqrt(squares / D + EPS)
    normed = (values * factor[:, None] * norm_gain.astype(jnp.float32)[None, :]).astype(
        jnp.bfloat16
    )
    rows = jnp.repeat(normed, 2, axis=0)
    buffer = jnp.zeros((experts * slot_cap, normed.shape[1]), jnp.bfloat16).at[target].set(rows)
    buffer = buffer.reshape(n_expdev, exp_local, slot_cap, normed.shape[1])
    arrived = lax.all_to_all(buffer, "ep", split_axis=0, concat_axis=0, tiled=True)
    piece = lax.all_gather(arrived, "tp", axis=3, tiled=True)
    first = jnp.einsum("secd,edf->secf", piece, gate_weight, preferred_element_type=jnp.float32)
    second = jnp.einsum("secd,edf->secf", piece, up_weight, preferred_element_type=jnp.float32)
    hidden = (jax.nn.silu(first) * second).astype(jnp.bfloat16)
    width_local = D // lax.axis_size("tp")
    term = jnp.einsum("secf,efd->dsec", hidden, down_weight, preferred_element_type=jnp.float32)
    summed = lax.psum_scatter(
        term.reshape(lax.axis_size("tp") * width_local, n_expdev * exp_local * slot_cap).astype(
            jnp.bfloat16
        ),
        "tp",
        scatter_dimension=0,
        tiled=True,
    )
    results = summed.reshape(width_local, n_expdev, exp_local, slot_cap)
    results = jnp.transpose(results, (1, 2, 3, 0))
    returned = lax.all_to_all(results, "ep", split_axis=0, concat_axis=0, tiled=True)
    flat_back = returned.reshape(experts * slot_cap, width_local)
    picked = flat_back[target].astype(jnp.float32).reshape(tok_rows, 2, width_local)
    return jnp.sum(picked * gate_share[:, :, None], axis=1).astype(jnp.bfloat16)


def fused(
    n, n_tp,
    tok_hbm, gain_hbm, ids_hbm, share_hbm, wg_hbm, wu_hbm, wd_hbm,
    out_ref,
    tok, gain, ids, share, wg, wu, wd, gains, slot_row, share_row, send_a, xs, block,
    hid, own_y, ys, yd, za, zs, zx, rs, ra, ns, na, away_part, far_part, sums, mix_hi, mix_lo,
    in_sem, w_sem, g_send, g_recv, a_send, a_recv,
    f_send, f_recv, d_send, d_recv, e_send, e_recv, y_send, y_recv, z_send, z_recv, r_send, r_recv,
    h_send, h_recv,
):
    me = lax.axis_index("ep")
    tp = lax.axis_index("tp")
    x, c = tp // CORES, tp % CORES
    partner = x * CORES + (1 - c)
    across = (1 - x) * CORES + c
    diag = (1 - x) * CORES + (1 - c)
    rows, width = tok.shape
    cap = send_a.shape[1]
    half = n // 2

    z, y = me // LINE, me % LINE
    depth = n // LINE
    high = z // (depth // 2)
    outer = (z + high + 1) % 2
    beside = z + 1 - 2 * (z % 2)
    inner_there = depth // 2 - high
    outer_there = (1 - high) * (depth - 1)

    def either(pair, value=lambda k: k):
        a, b = value(pair[0]), value(pair[1])
        return a if pair[0] == pair[1] else outer * a + (1 - outer) * b

    def peer_of(k):
        level = (z, beside, inner_there, outer_there)[k // LINE]
        return level * LINE + (1 - y if k % LINE else y)

    def there_of(k):
        return k if k < half else half + LINE * outer + k % LINE

    def at(k):
        return either(k)

    def peer(k):
        return either(k, peer_of)

    def there(k):
        return either(k, there_of)

    barrier = pltpu.get_barrier_semaphore()
    for k in range(1, n):
        pl.semaphore_signal(barrier, inc=1, device_id=(peer_of(k), tp), device_id_type=MESH)
    for other in (partner, across, diag):
        pl.semaphore_signal(barrier, inc=1, device_id=(me, other), device_id_type=MESH)

    inputs = [
        pltpu.make_async_copy(src, dst, in_sem.at[i])
        for i, (src, dst) in enumerate(
            ((tok_hbm, tok), (ids_hbm, ids), (share_hbm, share), (gain_hbm, gain))
        )
    ]
    for load in inputs:
        load.start()
    def remote(src, dst, ssem, rsem, e, t):
        return pltpu.make_async_remote_copy(
            src_ref=src, dst_ref=dst, send_sem=ssem, recv_sem=rsem,
            device_id=(e, t), device_id_type=MESH,
        )

    for load in inputs:
        load.wait()
    loads = [
        pltpu.make_async_copy(wg_hbm.at[0], wg, w_sem.at[0]),
        pltpu.make_async_copy(wu_hbm.at[0], wu, w_sem.at[1]),
    ] + [
        pltpu.make_async_copy(wd_hbm.at[0, :, pl.ds(q * width, width)], wd.at[q], w_sem.at[2 + q])
        for q in range(n_tp)
    ]

    experts = slot_row.shape[0]
    expert_of = lax.broadcasted_iota(jnp.int32, (experts, rows), 0)
    first = expert_of == ids[0:1, :]
    second = expert_of == ids[1:2, :]
    named = jnp.where(first | second, 1.0, 0.0)
    before = (
        lax.broadcasted_iota(jnp.int32, (rows, rows), 0)
        < lax.broadcasted_iota(jnp.int32, (rows, rows), 1)
    )
    earlier = jnp.dot(
        named.astype(BF), jnp.where(before, 1.0, 0.0).astype(BF), preferred_element_type=F32
    )
    slot_row[...] = jnp.where(named > 0.5, earlier, -1.0)
    share_row[...] = jnp.where(first, share[0:1, :], 0.0) + jnp.where(
        second, share[1:2, :], 0.0
    )
    slot_of = lax.broadcasted_iota(jnp.int32, (cap, rows), 0).astype(F32)

    def placed(k):
        return slot_of == jnp.broadcast_to(slot_row[pl.ds(peer(k), 1), :], (cap, rows))

    def place(k):
        return jnp.dot(
            jnp.where(placed(k), 1.0, 0.0).astype(BF), tok[...], preferred_element_type=F32
        ).astype(BF)

    def a_copy(k):
        s = there(k)
        return remote(
            send_a.at[at(k)], xs.at[s, c, x], a_send.at[at(k)], a_recv.at[s], peer(k), tp
        )

    def a_arrival(k):
        s = at(k)
        return remote(send_a.at[s], xs.at[s, c, x], a_send.at[s], a_recv.at[s], peer(k), tp)

    def send(k):
        send_a[at(k)] = place(k)
        a_copy(k).start()

    def f_copy(k):
        ref = xs.at[at(k), c, x]
        return remote(ref, ref, f_send.at[at(k)], f_recv.at[at(k)], me, across)

    def weigh(k):
        weight = jnp.where(
            placed(k), jnp.broadcast_to(share_row[pl.ds(peer(k), 1), :], (cap, rows)), 0.0
        )
        weight = jnp.transpose(weight)
        high_part = weight.astype(BF)
        mix_hi[at(k)] = high_part
        mix_lo[at(k)] = (weight - high_part.astype(F32)).astype(BF)

    sends = [slot_pair(word) for word in SENDS]
    ahead = sends[:2]
    for k in ahead:
        send_a[at(k)] = place(k)
    own = (0, 0)
    xs[0, c, x] = place(own)
    gains[pl.ds(tp, 1)] = jnp.broadcast_to(
        gain[...].astype(F32).reshape(1, 1, width), (1, 1, width)
    )

    with mark("barrier"):
        pl.semaphore_wait(barrier, n_tp - 1 + n - 1)
    g_copies = [
        remote(gains.at[tp], gains.at[tp], g_send.at[j], g_recv.at[j], me, other)
        for j, other in enumerate((partner, across, diag))
    ]
    g_arrivals = [
        remote(gains.at[other], gains.at[other], g_send.at[j], g_recv.at[j], me, other)
        for j, other in enumerate((partner, across, diag))
    ]
    for copy in g_copies:
        copy.start()
    for k in ahead:
        a_copy(k).start()
    f_copy(own).start()
    for k in sends[2:]:
        send(k)

    for load in loads:
        load.start()

    with mark("weigh"):
        for k in range(n):
            weigh((k, k))

    def f_arrival(k):
        ref = xs.at[at(k), c, 1 - x]
        return remote(ref, ref, f_send.at[at(k)], f_recv.at[at(k)], me, across)

    def d_copy(k, core):
        ref = xs.at[at(k), core, x]
        return remote(ref, ref, d_send.at[at(k)], d_recv.at[at(k)], me, partner)

    def e_copy(k, core):
        ref = xs.at[at(k), core, 1 - x]
        return remote(ref, ref, e_send.at[at(k)], e_recv.at[at(k)], me, partner)

    def y_copy(k):
        s = at(k)
        return remote(ys.at[s], yd.at[s], y_send.at[s], y_recv.at[s], me, partner)

    def z_copy(k):
        s = at(k)
        return remote(zs.at[s], zx.at[s], z_send.at[s], z_recv.at[s], me, across)

    def h_copy(k):
        s = at(k)
        return remote(ns.at[s], na.at[s], r_send.at[s], r_recv.at[s], peer(k), tp)

    x_copy = remote(away_part, far_part, h_send, h_recv, me, across)

    def home(k):
        s = at(k)
        y_copy(k).wait_recv()
        for i in (1, 0):
            result = (own_y[s, i] + yd[s, i].astype(F32)).astype(BF)
            if k == own:
                na[0, i] = result
            else:
                ns[s, i] = result
        if k != own:
            h_copy(k).start()

    def r_copy(k):
        s = there(k)
        return remote(rs.at[at(k)], ra.at[s], r_send.at[at(k)], r_recv.at[s], peer(k), tp)

    def r_arrival(k):
        s = at(k)
        return remote(rs.at[s], ra.at[s], r_send.at[s], r_recv.at[s], peer(k), tp)

    def take(k):
        if k != own:
            a_arrival(k).wait_recv()
            f_copy(k).start()
        d_copy(k, c).start()

    def pass_on(k):
        f_arrival(k).wait_recv()
        e_copy(k, c).start()

    def ready(k):
        d_copy(k, 1 - c).wait_recv()
        e_copy(k, 1 - c).wait_recv()

    def pair(k):
        s = at(k)
        y_copy(k).wait_recv()
        zs[s] = (own_y[s, 1] + yd[s, 1].astype(F32)).astype(BF)
        z_copy(k).start()
        za[s] = own_y[s, 0] + yd[s, 0].astype(F32)

    def give(k):
        s = at(k)
        z_copy(k).wait_recv()
        rs[s] = (za[s] + zx[s].astype(F32)).astype(BF)
        r_copy(k).start()

    ff = wg.shape[1]
    tile = 256 if ff % 256 == 0 else 128

    def normalize(k):
        s = at(k)
        pieces = [xs[s, q % CORES, q // CORES].astype(F32) for q in range(n_tp)]
        lanes = None
        for piece in pieces:
            square = piece * piece
            for j in range(0, width, 128):
                part = square[:, j:j + 128]
                lanes = part if lanes is None else lanes + part
        total = jnp.sum(lanes, axis=1, keepdims=True)
        factor = lax.rsqrt(total / (width * n_tp) + EPS)
        for q, piece in enumerate(pieces):
            block[:, q * width:(q + 1) * width] = (
                piece * factor * gains[q]
            ).astype(BF)

    def up_gate(k, part):
        for f in range(part * ff // 4, (part + 1) * ff // 4, tile):
            gate = jnp.dot(block[...], wg[:, f:f + tile], preferred_element_type=F32)
            up = jnp.dot(block[...], wu[:, f:f + tile], preferred_element_type=F32)
            hid[:, f:f + tile] = (gate / (1.0 + jnp.exp(-gate)) * up).astype(BF)

    def down_away(k):
        s = at(k)
        for i, q_x in ((1, 1 - x), (0, x)):
            ys[s, i] = jnp.dot(
                hid[...], wd[q_x * CORES + 1 - c], preferred_element_type=F32
            ).astype(BF)
        y_copy(k).start()

    def down_here(k):
        s = at(k)
        for i, q_x in ((1, 1 - x), (0, x)):
            own_y[s, i] = jnp.dot(hid[...], wd[q_x * CORES + c], preferred_element_type=F32)

    def mixed(k, back):
        return jnp.dot(mix_hi[at(k)], back, preferred_element_type=F32) + jnp.dot(
            mix_lo[at(k)], back, preferred_element_type=F32
        )

    def collect(k):
        h_copy(k).wait_recv()

    def swap(k):
        total = None
        for s in range(NEAR):
            part = mixed((s, s), na[s, 1])
            total = part if total is None else total + part
        away_part[...] = total.astype(BF)
        x_copy.start()

    def gather(k):
        total = None
        for s in range(NEAR):
            part = mixed((s, s), na[s, 0])
            total = part if total is None else total + part
        sums[...] = total

    def far_mix(k):
        r_arrival(k).wait_recv()
        sums[...] = sums[...] + mixed(k, ra[at(k)])

    with mark("gains"):
        for copy in g_arrivals:
            copy.wait_recv()

    def weights(k):
        for load in loads:
            load.wait()

    def only(role, action):
        def run(k):
            @pl.when(outer == role)
            def _():
                action(k)
        return run

    todo = {
        "take": take, "pass": pass_on, "ready": ready, "norm": normalize, "load": weights,
        "away": down_away, "here": down_here, "pair": pair, "give": give,
        "home": home, "collect": collect, "swap": swap, "gather": gather, "mix": far_mix,
    }
    for part in range(4):
        todo["gu%d" % part] = functools.partial(up_gate, part=part)
    for word in ORDER:
        name, ks = word.split(":")
        k = slot_pair(ks)
        action = todo[name.strip("<>")]
        if name[0] == "<":
            action = only(1, action)
        elif name[0] == ">":
            action = only(0, action)
        with mark("%s_%s" % (name, ks.replace("/", "i"))):
            action(k)

    last = slot_pair(LAST)
    with mark("last"):
        r_arrival(last).wait_recv()
    total = sums[...] + mixed(last, ra[at(last)])
    with mark("swapped"):
        x_copy.wait_recv()
    out_ref[...] = (total + far_part[...].astype(F32)).astype(BF)

    with mark("sends"):
        for copy in g_copies:
            copy.wait_send()
        for k in [(k, k) for k in range(n)]:
            f_copy(k).wait_send()
            d_copy(k, c).wait_send()
            e_copy(k, c).wait_send()
            y_copy(k).wait_send()
            if k != own:
                a_copy(k).wait_send()
            if k[0] >= NEAR:
                z_copy(k).wait_send()
                r_copy(k).wait_send()
            elif k != own:
                h_copy(k).wait_send()
        x_copy.wait_send()


def slot_pair(word):
    parts = word.split("/")
    return int(parts[0]), int(parts[-1])


def routed(n, n_tp, tokens, norm_gain, expert_ids, gate_share, gate_weight, up_weight, down_weight):
    rows, width = tokens.shape
    experts = n * gate_weight.shape[0]
    cap = 4 * rows // experts
    depth, ff = gate_weight.shape[1:]
    hbm = pl.BlockSpec(memory_space=pltpu.HBM)
    dma = pltpu.SemaphoreType.DMA
    return pl.pallas_call(
        functools.partial(fused, n, n_tp),
        out_shape=pltpu.VMEM((rows, width), BF),
        in_specs=[hbm] * 7,
        out_specs=pl.BlockSpec(memory_space=pltpu.VMEM),
        scratch_shapes=[
            pltpu.VMEM((rows, width), BF),
            pltpu.VMEM((width,), BF),
            pltpu.VMEM((2, rows), jnp.int32),
            pltpu.VMEM((2, rows), F32),
            pltpu.VMEM((depth, ff), BF),
            pltpu.VMEM((depth, ff), BF),
            pltpu.VMEM((n_tp, ff, width), BF),
            pltpu.VMEM((n_tp, 1, width), F32),
            pltpu.VMEM((experts, rows), F32),
            pltpu.VMEM((experts, rows), F32),
            pltpu.VMEM((n, cap, width), BF),
            pltpu.VMEM((n, CORES, n_tp // CORES, cap, width), BF),
            pltpu.VMEM((cap, depth), BF),
            pltpu.VMEM((cap, ff), BF),
            pltpu.VMEM((n, 2, cap, width), F32),
            pltpu.VMEM((n, 2, cap, width), BF),
            pltpu.VMEM((n, 2, cap, width), BF),
            pltpu.VMEM((n, cap, width), F32),
            pltpu.VMEM((n, cap, width), BF),
            pltpu.VMEM((n, cap, width), BF),
            pltpu.VMEM((n, cap, width), BF),
            pltpu.VMEM((n, cap, width), BF),
            pltpu.VMEM((n // 2, 2, cap, width), BF),
            pltpu.VMEM((n // 2, 2, cap, width), BF),
            pltpu.VMEM((rows, width), BF),
            pltpu.VMEM((rows, width), BF),
            pltpu.VMEM((rows, width), F32),
            pltpu.VMEM((n, rows, cap), BF),
            pltpu.VMEM((n, rows, cap), BF),
            dma((4,)), dma((2 + n_tp,)),
            dma((3,)), dma((3,)),
            dma((n,)), dma((n,)),
            dma((n,)), dma((n,)),
            dma((n,)), dma((n,)),
            dma((n,)), dma((n,)),
            dma((n,)), dma((n,)),
            dma((n,)), dma((n,)),
            dma((n,)), dma((n,)),
            dma, dma,
        ],
        compiler_params=pltpu.CompilerParams(
            collective_id=0, has_side_effects=True, vmem_limit_bytes=56 * 1024 * 1024
        ),
    )(
        tokens, norm_gain, expert_ids.T, gate_share.T,
        gate_weight, up_weight, down_weight,
    )


def shards(n, n_tp, *args):
    tokens, gate_weight = args[0], args[4]
    rows, width = tokens.shape
    cap = 4 * rows // (n * gate_weight.shape[0])
    fits = (
        n_tp == 2 * CORES and n == 4 * LINE and gate_weight.shape[0] == 1 and rows % 128 == 0
        and width % 128 == 0 and gate_weight.shape[2] % 128 == 0 and cap % 128 == 0
    )
    return routed(n, n_tp, *args) if fits else plain(*args)


def solution(mesh):
    body = functools.partial(shards, mesh.shape["ep"], mesh.shape["tp"])
    in_specs = (
        P("ep", "tp"),
        P("tp"),
        P("ep", None),
        P("ep", None),
        P("ep", None, "tp"),
        P("ep", None, "tp"),
        P("ep", "tp", None),
    )
    out_specs = P("ep", "tp")
    return jax.shard_map(body, mesh=mesh, in_specs=in_specs, out_specs=out_specs, check_vma=False)
```

```python
import functools
import jax
import jax.numpy as jnp
from jax import lax
from jax.experimental import pallas as pl
from jax.experimental.pallas import tpu as pltpu
from jax.sharding import PartitionSpec as P

D = 2048


EPS = 1e-06
MESH = pl.DeviceIdType.MESH
BF = jnp.bfloat16
F32 = jnp.float32
CORES = 2
LINE = 2
mark = jax.named_scope
SENDS = (
    "6/2", "4/3", "2/1", "3/4", "1/6", "7/5", "5/7",
)
NEAR = 3
LAST = "5"
ORDER = (
    "take:0", "take:1", "pass:0", "<take:6",
    "load:0", "ready:0", "norm:0", "gu0:0", "gu1:0", "gu2:0", "gu3:0", "away:0", "here:0",
    ">take:6", "<take:2", "pass:1",
    "ready:1", "norm:1", "gu0:1", "gu1:1", "home:0", "<take:3", ">take:4", "gu2:1", "gu3:1",
    "<pass:6", ">take:2", "away:1", "here:1", ">pass:6",
    "ready:6", "norm:6", "gu0:6", "home:1", "gu1:6", ">take:3", "gu2:6", "<take:4", "gu3:6",
    "pass:2/4", "away:6", "here:6",
    "ready:2/4", "norm:2/4", "gu0:2/4", "pair:6", "gu1:2/4", "gu2:2/4", "gu3:2/4", "pass:3/2",
    "away:2/4", "take:7", "here:2/4", "<pass:4",
    "ready:4/2", "norm:4/2", "gu0:4/2", "<home:2", ">take:5", ">pair:4", "gu1:4/2", "gu2:4/2",
    "gu3:4/2", ">pass:3", "away:4/2", "here:4/2", "<give:6", "<take:5",
    "ready:3", "norm:3", "gu0:3", "<pair:4", ">home:2", ">give:6", "gu1:3", "gu2:3", "gu3:3",
    ">pass:7", "away:3", "here:3", "<pass:7",
    "ready:7", "norm:7", "gu0:7", "pair:3", "gu1:7", "gu2:7", "gu3:7", "pass:5", "<give:4",
    "away:7", "here:7",
    "ready:5", "norm:5", "gu0:5", "pair:7", ">give:4", "gu1:5", "gu2:5", "gu3:5", "away:5",
    ">give:3", "here:5",
    "pair:5", "<give:3", "give:7", "collect:1", "collect:2", "swap:0", "give:5", "gather:0",
    "mix:6", "mix:4", "mix:3", "mix:7",
)


def plain(tokens, norm_gain, expert_ids, gate_share, gate_weight, up_weight, down_weight):
    n_expdev = lax.axis_size("ep")
    exp_local = gate_weight.shape[0]
    experts = exp_local * n_expdev
    tok_rows = tokens.shape[0]
    slot_cap = 4 * tok_rows // experts
    flat_ids = expert_ids.reshape(-1)
    onehot = (flat_ids[:, None] == jnp.arange(experts, dtype=jnp.int32)[None, :]).astype(jnp.int32)
    slots = jnp.sum((jnp.cumsum(onehot, axis=0) - onehot) * onehot, axis=1)
    target = flat_ids * slot_cap + slots
    values = tokens.astype(jnp.float32)
    squares = lax.psum(jnp.sum(values * values, axis=1), "tp")
    factor = lax.rsqrt(squares / D + EPS)
    normed = (values * factor[:, None] * norm_gain.astype(jnp.float32)[None, :]).astype(
        jnp.bfloat16
    )
    rows = jnp.repeat(normed, 2, axis=0)
    buffer = jnp.zeros((experts * slot_cap, normed.shape[1]), jnp.bfloat16).at[target].set(rows)
    buffer = buffer.reshape(n_expdev, exp_local, slot_cap, normed.shape[1])
    arrived = lax.all_to_all(buffer, "ep", split_axis=0, concat_axis=0, tiled=True)
    piece = lax.all_gather(arrived, "tp", axis=3, tiled=True)
    first = jnp.einsum("secd,edf->secf", piece, gate_weight, preferred_element_type=jnp.float32)
    second = jnp.einsum("secd,edf->secf", piece, up_weight, preferred_element_type=jnp.float32)
    hidden = (jax.nn.silu(first) * second).astype(jnp.bfloat16)
    width_local = D // lax.axis_size("tp")
    term = jnp.einsum("secf,efd->dsec", hidden, down_weight, preferred_element_type=jnp.float32)
    summed = lax.psum_scatter(
        term.reshape(lax.axis_size("tp") * width_local, n_expdev * exp_local * slot_cap).astype(
            jnp.bfloat16
        ),
        "tp",
        scatter_dimension=0,
        tiled=True,
    )
    results = summed.reshape(width_local, n_expdev, exp_local, slot_cap)
    results = jnp.transpose(results, (1, 2, 3, 0))
    returned = lax.all_to_all(results, "ep", split_axis=0, concat_axis=0, tiled=True)
    flat_back = returned.reshape(experts * slot_cap, width_local)
    picked = flat_back[target].astype(jnp.float32).reshape(tok_rows, 2, width_local)
    return jnp.sum(picked * gate_share[:, :, None], axis=1).astype(jnp.bfloat16)


def fused(
    n, n_tp,
    tok_hbm, gain_hbm, ids_hbm, share_hbm, wg_hbm, wu_hbm, wd_hbm,
    out_ref,
    tok, gain, ids, share, wg, wu, wd, gains, slot_row, share_row, send_a, xs, block,
    hid, own_y, ys, yd, za, zs, zx, rs, ra, ns, na, away_part, far_part, sums, mix_hi, mix_lo,
    in_sem, w_sem, g_send, g_recv, a_send, a_recv,
    f_send, f_recv, d_send, d_recv, e_send, e_recv, y_send, y_recv, z_send, z_recv, r_send, r_recv,
    h_send, h_recv, n_send,
):
    me = lax.axis_index("ep")
    tp = lax.axis_index("tp")
    x, c = tp // CORES, tp % CORES
    partner = x * CORES + (1 - c)
    across = (1 - x) * CORES + c
    diag = (1 - x) * CORES + (1 - c)
    rows, width = tok.shape
    cap = send_a.shape[1]
    half = n // 2

    z, y = me // LINE, me % LINE
    depth = n // LINE
    high = z // (depth // 2)
    outer = (z + high + 1) % 2
    beside = z + 1 - 2 * (z % 2)
    inner_there = depth // 2 - high
    outer_there = (1 - high) * (depth - 1)

    def either(pair, value=lambda k: k):
        a, b = value(pair[0]), value(pair[1])
        return a if pair[0] == pair[1] else outer * a + (1 - outer) * b

    def peer_of(k):
        level = (z, beside, inner_there, outer_there)[k // LINE]
        return level * LINE + (1 - y if k % LINE else y)

    def there_of(k):
        return k if k < half else half + LINE * outer + k % LINE

    def at(k):
        return either(k)

    def peer(k):
        return either(k, peer_of)

    def there(k):
        return either(k, there_of)

    barrier = pltpu.get_barrier_semaphore()
    for k in range(1, n):
        pl.semaphore_signal(barrier, inc=1, device_id=(peer_of(k), tp), device_id_type=MESH)
    for other in (partner, across, diag):
        pl.semaphore_signal(barrier, inc=1, device_id=(me, other), device_id_type=MESH)

    inputs = [
        pltpu.make_async_copy(src, dst, in_sem.at[i])
        for i, (src, dst) in enumerate(
            ((tok_hbm, tok), (ids_hbm, ids), (share_hbm, share), (gain_hbm, gain))
        )
    ]
    for load in inputs:
        load.start()
    def remote(src, dst, ssem, rsem, e, t):
        return pltpu.make_async_remote_copy(
            src_ref=src, dst_ref=dst, send_sem=ssem, recv_sem=rsem,
            device_id=(e, t), device_id_type=MESH,
        )

    for load in inputs:
        load.wait()
    loads = [
        pltpu.make_async_copy(wg_hbm.at[0], wg, w_sem.at[0]),
        pltpu.make_async_copy(wu_hbm.at[0], wu, w_sem.at[1]),
    ] + [
        pltpu.make_async_copy(wd_hbm.at[0, :, pl.ds(q * width, width)], wd.at[q], w_sem.at[2 + q])
        for q in range(n_tp)
    ]

    experts = slot_row.shape[0]
    expert_of = lax.broadcasted_iota(jnp.int32, (experts, rows), 0)
    first = expert_of == ids[0:1, :]
    second = expert_of == ids[1:2, :]
    named = jnp.where(first | second, 1.0, 0.0)
    before = (
        lax.broadcasted_iota(jnp.int32, (rows, rows), 0)
        < lax.broadcasted_iota(jnp.int32, (rows, rows), 1)
    )
    earlier = jnp.dot(
        named.astype(BF), jnp.where(before, 1.0, 0.0).astype(BF), preferred_element_type=F32
    )
    slot_row[...] = jnp.where(named > 0.5, earlier, -1.0)
    share_row[...] = jnp.where(first, share[0:1, :], 0.0) + jnp.where(
        second, share[1:2, :], 0.0
    )
    slot_of = lax.broadcasted_iota(jnp.int32, (cap, rows), 0).astype(F32)

    def placed(k):
        return slot_of == jnp.broadcast_to(slot_row[pl.ds(peer(k), 1), :], (cap, rows))

    def place(k):
        return jnp.dot(
            jnp.where(placed(k), 1.0, 0.0).astype(BF), tok[...], preferred_element_type=F32
        ).astype(BF)

    def a_copy(k):
        s = there(k)
        return remote(
            send_a.at[at(k)], xs.at[s, c, x], a_send, a_recv.at[s], peer(k), tp
        )

    def a_arrival(k):
        s = at(k)
        return remote(send_a.at[s], xs.at[s, c, x], a_send, a_recv.at[s], peer(k), tp)

    def send(k):
        send_a[at(k)] = place(k)
        a_copy(k).start()

    def f_copy(k):
        ref = xs.at[at(k), c, x]
        return remote(ref, ref, f_send, f_recv.at[at(k)], me, across)

    def weigh(k):
        weight = jnp.where(
            placed(k), jnp.broadcast_to(share_row[pl.ds(peer(k), 1), :], (cap, rows)), 0.0
        )
        weight = jnp.transpose(weight)
        high_part = weight.astype(BF)
        mix_hi[at(k)] = high_part
        mix_lo[at(k)] = (weight - high_part.astype(F32)).astype(BF)

    sends = [slot_pair(word) for word in SENDS]
    ahead = sends[:2]
    for k in ahead:
        send_a[at(k)] = place(k)
    own = (0, 0)
    xs[0, c, x] = place(own)
    gains[pl.ds(tp, 1)] = jnp.broadcast_to(
        gain[...].astype(F32).reshape(1, 1, width), (1, 1, width)
    )

    with mark("barrier"):
        pl.semaphore_wait(barrier, n_tp - 1 + n - 1)
    g_copies = [
        remote(gains.at[tp], gains.at[tp], g_send, g_recv.at[j], me, other)
        for j, other in enumerate((partner, across, diag))
    ]
    g_arrivals = [
        remote(gains.at[other], gains.at[other], g_send, g_recv.at[j], me, other)
        for j, other in enumerate((partner, across, diag))
    ]
    for copy in g_copies:
        copy.start()
    for k in ahead:
        a_copy(k).start()
    f_copy(own).start()
    for k in sends[2:]:
        send(k)

    for load in loads:
        load.start()

    with mark("weigh"):
        for k in range(n):
            weigh((k, k))

    def f_arrival(k):
        ref = xs.at[at(k), c, 1 - x]
        return remote(ref, ref, f_send, f_recv.at[at(k)], me, across)

    def d_copy(k, core):
        ref = xs.at[at(k), core, x]
        return remote(ref, ref, d_send, d_recv.at[at(k)], me, partner)

    def e_copy(k, core):
        ref = xs.at[at(k), core, 1 - x]
        return remote(ref, ref, e_send, e_recv.at[at(k)], me, partner)

    def y_copy(k):
        s = at(k)
        return remote(ys.at[s], yd.at[s], y_send, y_recv.at[s], me, partner)

    def z_copy(k):
        s = at(k)
        return remote(zs.at[s], zx.at[s], z_send, z_recv.at[s], me, across)

    def h_copy(k):
        s = at(k)
        return remote(ns.at[s], na.at[s], n_send, r_recv.at[s], peer(k), tp)

    x_copy = remote(away_part, far_part, h_send, h_recv, me, across)

    def home(k):
        s = at(k)
        y_copy(k).wait_recv()
        for i in (1, 0):
            result = (own_y[s, i] + yd[s, i].astype(F32)).astype(BF)
            if k == own:
                na[0, i] = result
            else:
                ns[s, i] = result
        if k != own:
            h_copy(k).start()

    def r_copy(k):
        s = there(k)
        return remote(rs.at[at(k)], ra.at[s], r_send, r_recv.at[s], peer(k), tp)

    def r_arrival(k):
        s = at(k)
        return remote(rs.at[s], ra.at[s], r_send, r_recv.at[s], peer(k), tp)

    def take(k):
        if k != own:
            a_arrival(k).wait_recv()
            f_copy(k).start()
        d_copy(k, c).start()

    def pass_on(k):
        f_arrival(k).wait_recv()
        e_copy(k, c).start()

    def ready(k):
        d_copy(k, 1 - c).wait_recv()
        e_copy(k, 1 - c).wait_recv()

    def pair(k):
        s = at(k)
        y_copy(k).wait_recv()
        zs[s] = (own_y[s, 1] + yd[s, 1].astype(F32)).astype(BF)
        z_copy(k).start()
        za[s] = own_y[s, 0] + yd[s, 0].astype(F32)

    def give(k):
        s = at(k)
        z_copy(k).wait_recv()
        rs[s] = (za[s] + zx[s].astype(F32)).astype(BF)
        r_copy(k).start()

    ff = wg.shape[1]
    tile = 256 if ff % 256 == 0 else 128

    def normalize(k):
        s = at(k)
        pieces = [xs[s, q % CORES, q // CORES].astype(F32) for q in range(n_tp)]
        lanes = None
        for piece in pieces:
            square = piece * piece
            for j in range(0, width, 128):
                part = square[:, j:j + 128]
                lanes = part if lanes is None else lanes + part
        total = jnp.sum(lanes, axis=1, keepdims=True)
        factor = lax.rsqrt(total / (width * n_tp) + EPS)
        for q, piece in enumerate(pieces):
            block[:, q * width:(q + 1) * width] = (
                piece * factor * gains[q]
            ).astype(BF)

    def up_gate(k, part):
        for f in range(part * ff // 4, (part + 1) * ff // 4, tile):
            gate = jnp.dot(block[...], wg[:, f:f + tile], preferred_element_type=F32)
            up = jnp.dot(block[...], wu[:, f:f + tile], preferred_element_type=F32)
            hid[:, f:f + tile] = (gate / (1.0 + jnp.exp(-gate)) * up).astype(BF)

    def down_away(k):
        s = at(k)
        for i, q_x in ((1, 1 - x), (0, x)):
            ys[s, i] = jnp.dot(
                hid[...], wd[q_x * CORES + 1 - c], preferred_element_type=F32
            ).astype(BF)
        y_copy(k).start()

    def down_here(k):
        s = at(k)
        for i, q_x in ((1, 1 - x), (0, x)):
            own_y[s, i] = jnp.dot(hid[...], wd[q_x * CORES + c], preferred_element_type=F32)

    def mixed(k, back):
        return jnp.dot(mix_hi[at(k)], back, preferred_element_type=F32) + jnp.dot(
            mix_lo[at(k)], back, preferred_element_type=F32
        )

    def collect(k):
        h_copy(k).wait_recv()

    def swap(k):
        total = None
        for s in range(NEAR):
            part = mixed((s, s), na[s, 1])
            total = part if total is None else total + part
        away_part[...] = total.astype(BF)
        x_copy.start()

    def gather(k):
        total = None
        for s in range(NEAR):
            part = mixed((s, s), na[s, 0])
            total = part if total is None else total + part
        sums[...] = total

    def far_mix(k):
        r_arrival(k).wait_recv()
        sums[...] = sums[...] + mixed(k, ra[at(k)])

    with mark("gains"):
        for copy in g_arrivals:
            copy.wait_recv()

    def weights(k):
        for load in loads:
            load.wait()

    def only(role, action):
        def run(k):
            @pl.when(outer == role)
            def _():
                action(k)
        return run

    todo = {
        "take": take, "pass": pass_on, "ready": ready, "norm": normalize, "load": weights,
        "away": down_away, "here": down_here, "pair": pair, "give": give,
        "home": home, "collect": collect, "swap": swap, "gather": gather, "mix": far_mix,
    }
    for part in range(4):
        todo["gu%d" % part] = functools.partial(up_gate, part=part)
    for word in ORDER:
        name, ks = word.split(":")
        k = slot_pair(ks)
        action = todo[name.strip("<>")]
        if name[0] == "<":
            action = only(1, action)
        elif name[0] == ">":
            action = only(0, action)
        with mark("%s_%s" % (name, ks.replace("/", "i"))):
            action(k)

    last = slot_pair(LAST)
    with mark("swapped"):
        x_copy.wait_recv()
    sums[...] = sums[...] + far_part[...].astype(F32)
    with mark("last"):
        r_arrival(last).wait_recv()
    out_ref[...] = (sums[...] + mixed(last, ra[at(last)])).astype(BF)

    with mark("sends"):
        mine, other = xs.at[:, c, x], xs.at[:, c, 1 - x]
        for ref, sem in (
            (send_a.at[pl.ds(1, n - 1)], a_send), (mine, f_send), (mine, d_send), (other, e_send),
            (ys, y_send), (zs.at[pl.ds(NEAR, n - NEAR)], z_send), (away_part, h_send),
            (rs.at[pl.ds(NEAR, n - NEAR)], r_send), (ns.at[pl.ds(1, NEAR - 1)], n_send),
            (gains.at[pl.ds(0, n_tp - 1)], g_send),
        ):
            remote(ref, ref, sem, h_recv, me, across).wait_send()


def slot_pair(word):
    parts = word.split("/")
    return int(parts[0]), int(parts[-1])


def routed(n, n_tp, tokens, norm_gain, expert_ids, gate_share, gate_weight, up_weight, down_weight):
    rows, width = tokens.shape
    experts = n * gate_weight.shape[0]
    cap = 4 * rows // experts
    depth, ff = gate_weight.shape[1:]
    hbm = pl.BlockSpec(memory_space=pltpu.HBM)
    dma = pltpu.SemaphoreType.DMA
    return pl.pallas_call(
        functools.partial(fused, n, n_tp),
        out_shape=pltpu.VMEM((rows, width), BF),
        in_specs=[hbm] * 7,
        out_specs=pl.BlockSpec(memory_space=pltpu.VMEM),
        scratch_shapes=[
            pltpu.VMEM((rows, width), BF),
            pltpu.VMEM((width,), BF),
            pltpu.VMEM((2, rows), jnp.int32),
            pltpu.VMEM((2, rows), F32),
            pltpu.VMEM((depth, ff), BF),
            pltpu.VMEM((depth, ff), BF),
            pltpu.VMEM((n_tp, ff, width), BF),
            pltpu.VMEM((n_tp, 1, width), F32),
            pltpu.VMEM((experts, rows), F32),
            pltpu.VMEM((experts, rows), F32),
            pltpu.VMEM((n, cap, width), BF),
            pltpu.VMEM((n, CORES, n_tp // CORES, cap, width), BF),
            pltpu.VMEM((cap, depth), BF),
            pltpu.VMEM((cap, ff), BF),
            pltpu.VMEM((n, 2, cap, width), F32),
            pltpu.VMEM((n, 2, cap, width), BF),
            pltpu.VMEM((n, 2, cap, width), BF),
            pltpu.VMEM((n, cap, width), F32),
            pltpu.VMEM((n, cap, width), BF),
            pltpu.VMEM((n, cap, width), BF),
            pltpu.VMEM((n, cap, width), BF),
            pltpu.VMEM((n, cap, width), BF),
            pltpu.VMEM((n // 2, 2, cap, width), BF),
            pltpu.VMEM((n // 2, 2, cap, width), BF),
            pltpu.VMEM((rows, width), BF),
            pltpu.VMEM((rows, width), BF),
            pltpu.VMEM((rows, width), F32),
            pltpu.VMEM((n, rows, cap), BF),
            pltpu.VMEM((n, rows, cap), BF),
            dma((4,)), dma((2 + n_tp,)),
            dma, dma((3,)),
            dma, dma((n,)),
            dma, dma((n,)),
            dma, dma((n,)),
            dma, dma((n,)),
            dma, dma((n,)),
            dma, dma((n,)),
            dma, dma((n,)),
            dma, dma, dma,
        ],
        compiler_params=pltpu.CompilerParams(
            collective_id=0, has_side_effects=True, vmem_limit_bytes=56 * 1024 * 1024
        ),
    )(
        tokens, norm_gain, expert_ids.T, gate_share.T,
        gate_weight, up_weight, down_weight,
    )


def shards(n, n_tp, *args):
    tokens, gate_weight = args[0], args[4]
    rows, width = tokens.shape
    cap = 4 * rows // (n * gate_weight.shape[0])
    fits = (
        n_tp == 2 * CORES and n == 4 * LINE and gate_weight.shape[0] == 1 and rows % 128 == 0
        and width % 128 == 0 and gate_weight.shape[2] % 128 == 0 and cap % 128 == 0
    )
    return routed(n, n_tp, *args) if fits else plain(*args)


def solution(mesh):
    body = functools.partial(shards, mesh.shape["ep"], mesh.shape["tp"])
    in_specs = (
        P("ep", "tp"),
        P("tp"),
        P("ep", None),
        P("ep", None),
        P("ep", None, "tp"),
        P("ep", None, "tp"),
        P("ep", "tp", None),
    )
    out_specs = P("ep", "tp")
    return jax.shard_map(body, mesh=mesh, in_specs=in_specs, out_specs=out_specs, check_vma=False)
```

```python
import functools
import jax
import jax.numpy as jnp
from jax import lax
from jax.experimental import pallas as pl
from jax.experimental.pallas import tpu as pltpu
from jax.sharding import PartitionSpec as P

D = 2048


EPS = 1e-06
MESH = pl.DeviceIdType.MESH
BF = jnp.bfloat16
F32 = jnp.float32
CORES = 2
LINE = 2
mark = jax.named_scope
SENDS = (
    "6/2", "4/3", "2/1", "3/4", "1/6", "7/5", "5/7",
)
NEAR = 3
LAST = "5"
ORDER = (
    "take:0", "take:1", "pass:0", "<take:6",
    "load:0", "ready:0", "norm:0", "gu0:0", "gu1:0", "gu2:0", "gu3:0", "away:0", "here:0",
    ">take:6", "<take:2", "pass:1",
    "ready:1", "norm:1", "gu0:1", "gu1:1", "home:0", "<take:3", ">take:4", "gu2:1", "gu3:1",
    "<pass:6", ">take:2", "away:1", "here:1", ">pass:6",
    "ready:6", "norm:6", "gu0:6", "home:1", "gu1:6", ">take:3", "gu2:6", "<take:4", "gu3:6",
    "pass:2/4", "away:6", "here:6",
    "ready:2/4", "norm:2/4", "gu0:2/4", "pair:6", "gu1:2/4", "gu2:2/4", "gu3:2/4", "pass:3/2",
    "away:2/4", "take:7", "here:2/4", "<pass:4",
    "ready:4/2", "norm:4/2", "gu0:4/2", "<home:2", ">take:5", ">pair:4", "gu1:4/2", "gu2:4/2",
    "gu3:4/2", ">pass:3", "away:4/2", "here:4/2", "<give:6", "<take:5",
    "ready:3", "norm:3", "gu0:3", "<pair:4", ">home:2", ">give:6", "gu1:3", "gu2:3", "gu3:3",
    ">pass:7", "away:3", "here:3", "<pass:7",
    "ready:7", "norm:7", "gu0:7", "<pair:3", "]pair:3", "gu1:7", "gu2:7", "gu3:7", "pass:5",
    "<give:4", "away:7", "here:7",
    "ready:5", "norm:5", "gu0:5", "pair:7", ">give:4", "gu1:5", "gu2:5", "gu3:5", "away:5",
    "]give:3", "here:5",
    "pair:5", "[pair:3", "<give:3", "give:7", "collect:1", "collect:2", "swap:0", "give:5",
    "[give:3", "gather:0", "mix:6", "mix:4", "mix:3", "mix:7",
)


def plain(tokens, norm_gain, expert_ids, gate_share, gate_weight, up_weight, down_weight):
    n_expdev = lax.axis_size("ep")
    exp_local = gate_weight.shape[0]
    experts = exp_local * n_expdev
    tok_rows = tokens.shape[0]
    slot_cap = 4 * tok_rows // experts
    flat_ids = expert_ids.reshape(-1)
    onehot = (flat_ids[:, None] == jnp.arange(experts, dtype=jnp.int32)[None, :]).astype(jnp.int32)
    slots = jnp.sum((jnp.cumsum(onehot, axis=0) - onehot) * onehot, axis=1)
    target = flat_ids * slot_cap + slots
    values = tokens.astype(jnp.float32)
    squares = lax.psum(jnp.sum(values * values, axis=1), "tp")
    factor = lax.rsqrt(squares / D + EPS)
    normed = (values * factor[:, None] * norm_gain.astype(jnp.float32)[None, :]).astype(
        jnp.bfloat16
    )
    rows = jnp.repeat(normed, 2, axis=0)
    buffer = jnp.zeros((experts * slot_cap, normed.shape[1]), jnp.bfloat16).at[target].set(rows)
    buffer = buffer.reshape(n_expdev, exp_local, slot_cap, normed.shape[1])
    arrived = lax.all_to_all(buffer, "ep", split_axis=0, concat_axis=0, tiled=True)
    piece = lax.all_gather(arrived, "tp", axis=3, tiled=True)
    first = jnp.einsum("secd,edf->secf", piece, gate_weight, preferred_element_type=jnp.float32)
    second = jnp.einsum("secd,edf->secf", piece, up_weight, preferred_element_type=jnp.float32)
    hidden = (jax.nn.silu(first) * second).astype(jnp.bfloat16)
    width_local = D // lax.axis_size("tp")
    term = jnp.einsum("secf,efd->dsec", hidden, down_weight, preferred_element_type=jnp.float32)
    summed = lax.psum_scatter(
        term.reshape(lax.axis_size("tp") * width_local, n_expdev * exp_local * slot_cap).astype(
            jnp.bfloat16
        ),
        "tp",
        scatter_dimension=0,
        tiled=True,
    )
    results = summed.reshape(width_local, n_expdev, exp_local, slot_cap)
    results = jnp.transpose(results, (1, 2, 3, 0))
    returned = lax.all_to_all(results, "ep", split_axis=0, concat_axis=0, tiled=True)
    flat_back = returned.reshape(experts * slot_cap, width_local)
    picked = flat_back[target].astype(jnp.float32).reshape(tok_rows, 2, width_local)
    return jnp.sum(picked * gate_share[:, :, None], axis=1).astype(jnp.bfloat16)


def fused(
    n, n_tp,
    tok_hbm, gain_hbm, ids_hbm, share_hbm, wg_hbm, wu_hbm, wd_hbm,
    out_ref,
    tok, gain, ids, share, wg, wu, wd, gains, slot_row, share_row, send_a, xs, block,
    hid, own_y, ys, yd, za, zs, zx, rs, ra, ns, na, away_part, far_part, sums, mix_hi, mix_lo,
    in_sem, w_sem, g_send, g_recv, a_send, a_recv,
    f_send, f_recv, d_send, d_recv, e_send, e_recv, y_send, y_recv, z_send, z_recv, r_send, r_recv,
    h_send, h_recv, n_send,
):
    me = lax.axis_index("ep")
    tp = lax.axis_index("tp")
    x, c = tp // CORES, tp % CORES
    partner = x * CORES + (1 - c)
    across = (1 - x) * CORES + c
    diag = (1 - x) * CORES + (1 - c)
    rows, width = tok.shape
    cap = send_a.shape[1]
    half = n // 2

    z, y = me // LINE, me % LINE
    depth = n // LINE
    high = z // (depth // 2)
    outer = (z + high + 1) % 2
    beside = z + 1 - 2 * (z % 2)
    inner_there = depth // 2 - high
    outer_there = (1 - high) * (depth - 1)

    def either(pair, value=lambda k: k):
        a, b = value(pair[0]), value(pair[1])
        return a if pair[0] == pair[1] else outer * a + (1 - outer) * b

    def peer_of(k):
        level = (z, beside, inner_there, outer_there)[k // LINE]
        return level * LINE + (1 - y if k % LINE else y)

    def there_of(k):
        return k if k < half else half + LINE * outer + k % LINE

    def at(k):
        return either(k)

    def peer(k):
        return either(k, peer_of)

    def there(k):
        return either(k, there_of)

    barrier = pltpu.get_barrier_semaphore()
    for k in range(1, n):
        pl.semaphore_signal(barrier, inc=1, device_id=(peer_of(k), tp), device_id_type=MESH)
    for other in (partner, across, diag):
        pl.semaphore_signal(barrier, inc=1, device_id=(me, other), device_id_type=MESH)

    inputs = [
        pltpu.make_async_copy(src, dst, in_sem.at[i])
        for i, (src, dst) in enumerate(
            ((tok_hbm, tok), (ids_hbm, ids), (share_hbm, share), (gain_hbm, gain))
        )
    ]
    for load in inputs:
        load.start()
    def remote(src, dst, ssem, rsem, e, t):
        return pltpu.make_async_remote_copy(
            src_ref=src, dst_ref=dst, send_sem=ssem, recv_sem=rsem,
            device_id=(e, t), device_id_type=MESH,
        )

    for load in inputs:
        load.wait()
    loads = [
        pltpu.make_async_copy(wg_hbm.at[0], wg, w_sem.at[0]),
        pltpu.make_async_copy(wu_hbm.at[0], wu, w_sem.at[1]),
    ] + [
        pltpu.make_async_copy(wd_hbm.at[0, :, pl.ds(q * width, width)], wd.at[q], w_sem.at[2 + q])
        for q in range(n_tp)
    ]

    experts = slot_row.shape[0]
    expert_of = lax.broadcasted_iota(jnp.int32, (experts, rows), 0)
    first = expert_of == ids[0:1, :]
    second = expert_of == ids[1:2, :]
    named = jnp.where(first | second, 1.0, 0.0)
    before = (
        lax.broadcasted_iota(jnp.int32, (rows, rows), 0)
        < lax.broadcasted_iota(jnp.int32, (rows, rows), 1)
    )
    earlier = jnp.dot(
        named.astype(BF), jnp.where(before, 1.0, 0.0).astype(BF), preferred_element_type=F32
    )
    slot_row[...] = jnp.where(named > 0.5, earlier, -1.0)
    share_row[...] = jnp.where(first, share[0:1, :], 0.0) + jnp.where(
        second, share[1:2, :], 0.0
    )
    slot_of = lax.broadcasted_iota(jnp.int32, (cap, rows), 0).astype(F32)

    def placed(k):
        return slot_of == jnp.broadcast_to(slot_row[pl.ds(peer(k), 1), :], (cap, rows))

    def place(k):
        return jnp.dot(
            jnp.where(placed(k), 1.0, 0.0).astype(BF), tok[...], preferred_element_type=F32
        ).astype(BF)

    def a_copy(k):
        s = there(k)
        return remote(
            send_a.at[at(k)], xs.at[s, c, x], a_send, a_recv.at[s], peer(k), tp
        )

    def a_arrival(k):
        s = at(k)
        return remote(send_a.at[s], xs.at[s, c, x], a_send, a_recv.at[s], peer(k), tp)

    def send(k):
        send_a[at(k)] = place(k)
        a_copy(k).start()

    def f_copy(k):
        ref = xs.at[at(k), c, x]
        return remote(ref, ref, f_send, f_recv.at[at(k)], me, across)

    def weigh(k):
        weight = jnp.where(
            placed(k), jnp.broadcast_to(share_row[pl.ds(peer(k), 1), :], (cap, rows)), 0.0
        )
        weight = jnp.transpose(weight)
        high_part = weight.astype(BF)
        mix_hi[at(k)] = high_part
        mix_lo[at(k)] = (weight - high_part.astype(F32)).astype(BF)

    sends = [slot_pair(word) for word in SENDS]
    ahead = sends[:2]
    for k in ahead:
        send_a[at(k)] = place(k)
    own = (0, 0)
    xs[0, c, x] = place(own)
    gains[pl.ds(tp, 1)] = jnp.broadcast_to(
        gain[...].astype(F32).reshape(1, 1, width), (1, 1, width)
    )

    with mark("barrier"):
        pl.semaphore_wait(barrier, n_tp - 1 + n - 1)
    g_copies = [
        remote(gains.at[tp], gains.at[tp], g_send, g_recv.at[j], me, other)
        for j, other in enumerate((partner, across, diag))
    ]
    g_arrivals = [
        remote(gains.at[other], gains.at[other], g_send, g_recv.at[j], me, other)
        for j, other in enumerate((partner, across, diag))
    ]
    for copy in g_copies:
        copy.start()
    for k in ahead:
        a_copy(k).start()
    f_copy(own).start()
    for k in sends[2:]:
        send(k)

    for load in loads:
        load.start()

    with mark("weigh"):
        for k in range(n):
            weigh((k, k))

    def f_arrival(k):
        ref = xs.at[at(k), c, 1 - x]
        return remote(ref, ref, f_send, f_recv.at[at(k)], me, across)

    def d_copy(k, core):
        ref = xs.at[at(k), core, x]
        return remote(ref, ref, d_send, d_recv.at[at(k)], me, partner)

    def e_copy(k, core):
        ref = xs.at[at(k), core, 1 - x]
        return remote(ref, ref, e_send, e_recv.at[at(k)], me, partner)

    def y_copy(k):
        s = at(k)
        return remote(ys.at[s], yd.at[s], y_send, y_recv.at[s], me, partner)

    def z_copy(k):
        s = at(k)
        return remote(zs.at[s], zx.at[s], z_send, z_recv.at[s], me, across)

    def h_copy(k):
        s = at(k)
        return remote(ns.at[s], na.at[s], n_send, r_recv.at[s], peer(k), tp)

    x_copy = remote(away_part, far_part, h_send, h_recv, me, across)

    def home(k):
        s = at(k)
        y_copy(k).wait_recv()
        for i in (1, 0):
            result = (own_y[s, i] + yd[s, i].astype(F32)).astype(BF)
            if k == own:
                na[0, i] = result
            else:
                ns[s, i] = result
        if k != own:
            h_copy(k).start()

    def r_copy(k):
        s = there(k)
        return remote(rs.at[at(k)], ra.at[s], r_send, r_recv.at[s], peer(k), tp)

    def r_arrival(k):
        s = at(k)
        return remote(rs.at[s], ra.at[s], r_send, r_recv.at[s], peer(k), tp)

    def take(k):
        if k != own:
            a_arrival(k).wait_recv()
            f_copy(k).start()
        d_copy(k, c).start()

    def pass_on(k):
        f_arrival(k).wait_recv()
        e_copy(k, c).start()

    def ready(k):
        d_copy(k, 1 - c).wait_recv()
        e_copy(k, 1 - c).wait_recv()

    def pair(k):
        s = at(k)
        y_copy(k).wait_recv()
        zs[s] = (own_y[s, 1] + yd[s, 1].astype(F32)).astype(BF)
        z_copy(k).start()
        za[s] = own_y[s, 0] + yd[s, 0].astype(F32)

    def give(k):
        s = at(k)
        z_copy(k).wait_recv()
        rs[s] = (za[s] + zx[s].astype(F32)).astype(BF)
        r_copy(k).start()

    ff = wg.shape[1]
    tile = 256 if ff % 256 == 0 else 128

    def normalize(k):
        s = at(k)
        pieces = [xs[s, q % CORES, q // CORES].astype(F32) for q in range(n_tp)]
        lanes = None
        for piece in pieces:
            square = piece * piece
            for j in range(0, width, 128):
                part = square[:, j:j + 128]
                lanes = part if lanes is None else lanes + part
        total = jnp.sum(lanes, axis=1, keepdims=True)
        factor = lax.rsqrt(total / (width * n_tp) + EPS)
        for q, piece in enumerate(pieces):
            block[:, q * width:(q + 1) * width] = (
                piece * factor * gains[q]
            ).astype(BF)

    def up_gate(k, part):
        for f in range(part * ff // 4, (part + 1) * ff // 4, tile):
            gate = jnp.dot(block[...], wg[:, f:f + tile], preferred_element_type=F32)
            up = jnp.dot(block[...], wu[:, f:f + tile], preferred_element_type=F32)
            hid[:, f:f + tile] = (gate / (1.0 + jnp.exp(-gate)) * up).astype(BF)

    def down_away(k):
        s = at(k)
        for i, q_x in ((1, 1 - x), (0, x)):
            ys[s, i] = jnp.dot(
                hid[...], wd[q_x * CORES + 1 - c], preferred_element_type=F32
            ).astype(BF)
        y_copy(k).start()

    def down_here(k):
        s = at(k)
        for i, q_x in ((1, 1 - x), (0, x)):
            own_y[s, i] = jnp.dot(hid[...], wd[q_x * CORES + c], preferred_element_type=F32)

    def mixed(k, back):
        return jnp.dot(mix_hi[at(k)], back, preferred_element_type=F32) + jnp.dot(
            mix_lo[at(k)], back, preferred_element_type=F32
        )

    def collect(k):
        h_copy(k).wait_recv()

    def swap(k):
        total = None
        for s in range(NEAR):
            part = mixed((s, s), na[s, 1])
            total = part if total is None else total + part
        away_part[...] = total.astype(BF)
        x_copy.start()

    def gather(k):
        total = None
        for s in range(NEAR):
            part = mixed((s, s), na[s, 0])
            total = part if total is None else total + part
        sums[...] = total

    def far_mix(k):
        r_arrival(k).wait_recv()
        sums[...] = sums[...] + mixed(k, ra[at(k)])

    with mark("gains"):
        for copy in g_arrivals:
            copy.wait_recv()

    def weights(k):
        for load in loads:
            load.wait()

    def only(where, action):
        def run(k):
            @pl.when(where)
            def _():
                action(k)
        return run

    places = {
        "<": outer == 1, ">": outer == 0, "{": outer + high == 2, "}": outer - high == 1,
        "[": outer - high == -1, "]": outer + high == 0,
    }
    todo = {
        "take": take, "pass": pass_on, "ready": ready, "norm": normalize, "load": weights,
        "away": down_away, "here": down_here, "pair": pair, "give": give,
        "home": home, "collect": collect, "swap": swap, "gather": gather, "mix": far_mix,
    }
    for part in range(4):
        todo["gu%d" % part] = functools.partial(up_gate, part=part)
    for word in ORDER:
        name, ks = word.split(":")
        k = slot_pair(ks)
        action = todo[name.strip("<>{}[]")]
        if name[0] in places:
            action = only(places[name[0]], action)
        with mark("%s_%s" % (name, ks.replace("/", "i"))):
            action(k)

    last = slot_pair(LAST)
    with mark("swapped"):
        x_copy.wait_recv()
    sums[...] = sums[...] + far_part[...].astype(F32)
    with mark("last"):
        r_arrival(last).wait_recv()
    out_ref[...] = (sums[...] + mixed(last, ra[at(last)])).astype(BF)

    with mark("sends"):
        mine, other = xs.at[:, c, x], xs.at[:, c, 1 - x]
        for ref, sem in (
            (send_a.at[pl.ds(1, n - 1)], a_send), (mine, f_send), (mine, d_send), (other, e_send),
            (ys, y_send), (zs.at[pl.ds(NEAR, n - NEAR)], z_send), (away_part, h_send),
            (rs.at[pl.ds(NEAR, n - NEAR)], r_send), (ns.at[pl.ds(1, NEAR - 1)], n_send),
            (gains.at[pl.ds(0, n_tp - 1)], g_send),
        ):
            remote(ref, ref, sem, h_recv, me, across).wait_send()


def slot_pair(word):
    parts = word.split("/")
    return int(parts[0]), int(parts[-1])


def routed(n, n_tp, tokens, norm_gain, expert_ids, gate_share, gate_weight, up_weight, down_weight):
    rows, width = tokens.shape
    experts = n * gate_weight.shape[0]
    cap = 4 * rows // experts
    depth, ff = gate_weight.shape[1:]
    hbm = pl.BlockSpec(memory_space=pltpu.HBM)
    dma = pltpu.SemaphoreType.DMA
    return pl.pallas_call(
        functools.partial(fused, n, n_tp),
        out_shape=pltpu.VMEM((rows, width), BF),
        in_specs=[hbm] * 7,
        out_specs=pl.BlockSpec(memory_space=pltpu.VMEM),
        scratch_shapes=[
            pltpu.VMEM((rows, width), BF),
            pltpu.VMEM((width,), BF),
            pltpu.VMEM((2, rows), jnp.int32),
            pltpu.VMEM((2, rows), F32),
            pltpu.VMEM((depth, ff), BF),
            pltpu.VMEM((depth, ff), BF),
            pltpu.VMEM((n_tp, ff, width), BF),
            pltpu.VMEM((n_tp, 1, width), F32),
            pltpu.VMEM((experts, rows), F32),
            pltpu.VMEM((experts, rows), F32),
            pltpu.VMEM((n, cap, width), BF),
            pltpu.VMEM((n, CORES, n_tp // CORES, cap, width), BF),
            pltpu.VMEM((cap, depth), BF),
            pltpu.VMEM((cap, ff), BF),
            pltpu.VMEM((n, 2, cap, width), F32),
            pltpu.VMEM((n, 2, cap, width), BF),
            pltpu.VMEM((n, 2, cap, width), BF),
            pltpu.VMEM((n, cap, width), F32),
            pltpu.VMEM((n, cap, width), BF),
            pltpu.VMEM((n, cap, width), BF),
            pltpu.VMEM((n, cap, width), BF),
            pltpu.VMEM((n, cap, width), BF),
            pltpu.VMEM((n // 2, 2, cap, width), BF),
            pltpu.VMEM((n // 2, 2, cap, width), BF),
            pltpu.VMEM((rows, width), BF),
            pltpu.VMEM((rows, width), BF),
            pltpu.VMEM((rows, width), F32),
            pltpu.VMEM((n, rows, cap), BF),
            pltpu.VMEM((n, rows, cap), BF),
            dma((4,)), dma((2 + n_tp,)),
            dma, dma((3,)),
            dma, dma((n,)),
            dma, dma((n,)),
            dma, dma((n,)),
            dma, dma((n,)),
            dma, dma((n,)),
            dma, dma((n,)),
            dma, dma((n,)),
            dma, dma, dma,
        ],
        compiler_params=pltpu.CompilerParams(
            collective_id=0, has_side_effects=True, vmem_limit_bytes=56 * 1024 * 1024
        ),
    )(
        tokens, norm_gain, expert_ids.T, gate_share.T,
        gate_weight, up_weight, down_weight,
    )


def shards(n, n_tp, *args):
    tokens, gate_weight = args[0], args[4]
    rows, width = tokens.shape
    cap = 4 * rows // (n * gate_weight.shape[0])
    fits = (
        n_tp == 2 * CORES and n == 4 * LINE and gate_weight.shape[0] == 1 and rows % 128 == 0
        and width % 128 == 0 and gate_weight.shape[2] % 128 == 0 and cap % 128 == 0
    )
    return routed(n, n_tp, *args) if fits else plain(*args)


def solution(mesh):
    body = functools.partial(shards, mesh.shape["ep"], mesh.shape["tp"])
    in_specs = (
        P("ep", "tp"),
        P("tp"),
        P("ep", None),
        P("ep", None),
        P("ep", None, "tp"),
        P("ep", None, "tp"),
        P("ep", "tp", None),
    )
    out_specs = P("ep", "tp")
    return jax.shard_map(body, mesh=mesh, in_specs=in_specs, out_specs=out_specs, check_vma=False)
```

```python
import functools
import jax
import jax.numpy as jnp
from jax import lax
from jax.experimental import pallas as pl
from jax.experimental.pallas import tpu as pltpu
from jax.sharding import PartitionSpec as P

D = 2048


EPS = 1e-06
MESH = pl.DeviceIdType.MESH
BF = jnp.bfloat16
F32 = jnp.float32
CORES = 2
LINE = 2
mark = jax.named_scope
SENDS = (
    "6/2", "4/3", "2/1", "3/4", "1/6", "7/5", "5/7",
)
NEAR = 3
LAST = "5"
ORDER = (
    "take:0", "take:1", "pass:0", "<take:6",
    "load:0", "ready:0", "norm:0", "gu0:0", "gu1:0", "gu2:0", "gu3:0", "away:0", "here:0",
    ">take:6", "<take:2", "pass:1",
    "ready:1", "norm:1", "gu0:1", "gu1:1", "home:0", "<take:3", ">take:4", "gu2:1", "gu3:1",
    "<pass:6", ">take:2", "away:1", "here:1", ">pass:6",
    "ready:6", "norm:6", "gu0:6", "home:1", "gu1:6", ">take:3", "gu2:6", "<take:4", "gu3:6",
    "pass:2/4", "away:6", "here:6",
    "ready:2/4", "norm:2/4", "gu0:2/4", "pair:6", "gu1:2/4", "gu2:2/4", "gu3:2/4", "pass:3/2",
    "away:2/4", "take:7", "here:2/4", "<pass:4",
    "ready:4/2", "norm:4/2", "gu0:4/2", "<home:2", ">take:5", ">pair:4", "gu1:4/2", "gu2:4/2",
    "gu3:4/2", ">pass:3", "away:4/2", "here:4/2", "<give:6", "<take:5",
    "ready:3", "norm:3", "gu0:3", "<pair:4", ">home:2", ">give:6", "gu1:3", "gu2:3", "gu3:3",
    ">pass:7", "away:3", "here:3", "<pass:7",
    "ready:7", "norm:7", "gu0:7", "<pair:3", "]pair:3", "gu1:7", "gu2:7", "gu3:7", "pass:5",
    "<give:4", "away:7", "here:7",
    "ready:5", "norm:5", "gu0:5", "pair:7", ">give:4", "gu1:5", "gu2:5", "gu3:5", "away:5",
    "]give:3", "here:5",
    "pair:5", "[pair:3", "<give:3", "give:7", "collect:1", "collect:2", "swap:0", "give:5",
    "[give:3", "gather:0", "mix:6", "mix:4", "mix:3", "mix:7",
)


def plain(tokens, norm_gain, expert_ids, gate_share, gate_weight, up_weight, down_weight):
    n_expdev = lax.axis_size("ep")
    exp_local = gate_weight.shape[0]
    experts = exp_local * n_expdev
    tok_rows = tokens.shape[0]
    slot_cap = 4 * tok_rows // experts
    flat_ids = expert_ids.reshape(-1)
    onehot = (flat_ids[:, None] == jnp.arange(experts, dtype=jnp.int32)[None, :]).astype(jnp.int32)
    slots = jnp.sum((jnp.cumsum(onehot, axis=0) - onehot) * onehot, axis=1)
    target = flat_ids * slot_cap + slots
    values = tokens.astype(jnp.float32)
    squares = lax.psum(jnp.sum(values * values, axis=1), "tp")
    factor = lax.rsqrt(squares / D + EPS)
    normed = (values * factor[:, None] * norm_gain.astype(jnp.float32)[None, :]).astype(
        jnp.bfloat16
    )
    rows = jnp.repeat(normed, 2, axis=0)
    buffer = jnp.zeros((experts * slot_cap, normed.shape[1]), jnp.bfloat16).at[target].set(rows)
    buffer = buffer.reshape(n_expdev, exp_local, slot_cap, normed.shape[1])
    arrived = lax.all_to_all(buffer, "ep", split_axis=0, concat_axis=0, tiled=True)
    piece = lax.all_gather(arrived, "tp", axis=3, tiled=True)
    first = jnp.einsum("secd,edf->secf", piece, gate_weight, preferred_element_type=jnp.float32)
    second = jnp.einsum("secd,edf->secf", piece, up_weight, preferred_element_type=jnp.float32)
    hidden = (jax.nn.silu(first) * second).astype(jnp.bfloat16)
    width_local = D // lax.axis_size("tp")
    term = jnp.einsum("secf,efd->dsec", hidden, down_weight, preferred_element_type=jnp.float32)
    summed = lax.psum_scatter(
        term.reshape(lax.axis_size("tp") * width_local, n_expdev * exp_local * slot_cap).astype(
            jnp.bfloat16
        ),
        "tp",
        scatter_dimension=0,
        tiled=True,
    )
    results = summed.reshape(width_local, n_expdev, exp_local, slot_cap)
    results = jnp.transpose(results, (1, 2, 3, 0))
    returned = lax.all_to_all(results, "ep", split_axis=0, concat_axis=0, tiled=True)
    flat_back = returned.reshape(experts * slot_cap, width_local)
    picked = flat_back[target].astype(jnp.float32).reshape(tok_rows, 2, width_local)
    return jnp.sum(picked * gate_share[:, :, None], axis=1).astype(jnp.bfloat16)


def fused(
    n, n_tp,
    tok_hbm, gain_hbm, ids_hbm, share_hbm, wg_hbm, wu_hbm, wd_hbm,
    out_ref,
    tok, gain, ids, share, wg, wu, wd, gains, slot_row, share_row, send_a, xs, block,
    hid, own_y, ys, yd, za, zs, zx, rs, ra, ns, na, away_part, far_part, sums, mix_hi, mix_lo,
    in_sem, w_sem, g_send, g_recv, a_send, a_recv,
    f_send, f_recv, d_send, d_recv, e_send, e_recv, y_send, z_send, r_send, r_recv,
    h_send, h_recv, n_send,
):
    me = lax.axis_index("ep")
    tp = lax.axis_index("tp")
    x, c = tp // CORES, tp % CORES
    partner = x * CORES + (1 - c)
    across = (1 - x) * CORES + c
    diag = (1 - x) * CORES + (1 - c)
    rows, width = tok.shape
    cap = send_a.shape[1]
    half = n // 2

    z, y = me // LINE, me % LINE
    depth = n // LINE
    high = z // (depth // 2)
    outer = (z + high + 1) % 2
    beside = z + 1 - 2 * (z % 2)
    inner_there = depth // 2 - high
    outer_there = (1 - high) * (depth - 1)

    def either(pair, value=lambda k: k):
        a, b = value(pair[0]), value(pair[1])
        return a if pair[0] == pair[1] else outer * a + (1 - outer) * b

    def peer_of(k):
        level = (z, beside, inner_there, outer_there)[k // LINE]
        return level * LINE + (1 - y if k % LINE else y)

    def there_of(k):
        return k if k < half else half + LINE * outer + k % LINE

    def at(k):
        return either(k)

    def peer(k):
        return either(k, peer_of)

    def there(k):
        return either(k, there_of)

    barrier = pltpu.get_barrier_semaphore()
    for k in range(1, n):
        pl.semaphore_signal(barrier, inc=1, device_id=(peer_of(k), tp), device_id_type=MESH)
    for other in (partner, across, diag):
        pl.semaphore_signal(barrier, inc=1, device_id=(me, other), device_id_type=MESH)

    inputs = [
        pltpu.make_async_copy(src, dst, in_sem.at[i])
        for i, (src, dst) in enumerate(
            ((tok_hbm, tok), (ids_hbm, ids), (share_hbm, share), (gain_hbm, gain))
        )
    ]
    for load in inputs:
        load.start()
    def remote(src, dst, ssem, rsem, e, t):
        return pltpu.make_async_remote_copy(
            src_ref=src, dst_ref=dst, send_sem=ssem, recv_sem=rsem,
            device_id=(e, t), device_id_type=MESH,
        )

    for load in inputs:
        load.wait()
    loads = [
        pltpu.make_async_copy(wg_hbm.at[0], wg, w_sem.at[0]),
        pltpu.make_async_copy(wu_hbm.at[0], wu, w_sem.at[1]),
    ] + [
        pltpu.make_async_copy(wd_hbm.at[0, :, pl.ds(q * width, width)], wd.at[q], w_sem.at[2 + q])
        for q in range(n_tp)
    ]

    experts = slot_row.shape[0]
    expert_of = lax.broadcasted_iota(jnp.int32, (experts, rows), 0)
    first = expert_of == ids[0:1, :]
    second = expert_of == ids[1:2, :]
    named = jnp.where(first | second, 1.0, 0.0)
    before = (
        lax.broadcasted_iota(jnp.int32, (rows, rows), 0)
        < lax.broadcasted_iota(jnp.int32, (rows, rows), 1)
    )
    earlier = jnp.dot(
        named.astype(BF), jnp.where(before, 1.0, 0.0).astype(BF), preferred_element_type=F32
    )
    slot_row[...] = jnp.where(named > 0.5, earlier, -1.0)
    share_row[...] = jnp.where(first, share[0:1, :], 0.0) + jnp.where(
        second, share[1:2, :], 0.0
    )
    slot_of = lax.broadcasted_iota(jnp.int32, (cap, rows), 0).astype(F32)

    def placed(k):
        return slot_of == jnp.broadcast_to(slot_row[pl.ds(peer(k), 1), :], (cap, rows))

    def place(k):
        return jnp.dot(
            jnp.where(placed(k), 1.0, 0.0).astype(BF), tok[...], preferred_element_type=F32
        ).astype(BF)

    def a_copy(k):
        s = there(k)
        return remote(
            send_a.at[at(k)], xs.at[s, c, x], a_send, a_recv.at[s], peer(k), tp
        )

    def a_arrival(k):
        s = at(k)
        return remote(send_a.at[s], xs.at[s, c, x], a_send, a_recv.at[s], peer(k), tp)

    def send(k):
        send_a[at(k)] = place(k)
        a_copy(k).start()

    def f_copy(k):
        ref = xs.at[at(k), c, x]
        return remote(ref, ref, f_send, f_recv.at[at(k)], me, across)

    def weigh(k):
        weight = jnp.where(
            placed(k), jnp.broadcast_to(share_row[pl.ds(peer(k), 1), :], (cap, rows)), 0.0
        )
        weight = jnp.transpose(weight)
        high_part = weight.astype(BF)
        mix_hi[at(k)] = high_part
        mix_lo[at(k)] = (weight - high_part.astype(F32)).astype(BF)

    sends = [slot_pair(word) for word in SENDS]
    ahead = sends[:2]
    for k in ahead:
        send_a[at(k)] = place(k)
    own = (0, 0)
    xs[0, c, x] = place(own)
    gains[pl.ds(tp, 1)] = jnp.broadcast_to(
        gain[...].astype(F32).reshape(1, 1, width), (1, 1, width)
    )

    with mark("barrier"):
        pl.semaphore_wait(barrier, n_tp - 1 + n - 1)
    g_copies = [
        remote(gains.at[tp], gains.at[tp], g_send, g_recv.at[j], me, other)
        for j, other in enumerate((partner, across, diag))
    ]
    g_arrivals = [
        remote(gains.at[other], gains.at[other], g_send, g_recv.at[j], me, other)
        for j, other in enumerate((partner, across, diag))
    ]
    for copy in g_copies:
        copy.start()
    for k in ahead:
        a_copy(k).start()
    f_copy(own).start()
    for k in sends[2:]:
        send(k)

    for load in loads:
        load.start()

    with mark("weigh"):
        for k in range(n):
            weigh((k, k))

    def f_arrival(k):
        ref = xs.at[at(k), c, 1 - x]
        return remote(ref, ref, f_send, f_recv.at[at(k)], me, across)

    def d_copy(k, core):
        ref = xs.at[at(k), core, x]
        return remote(ref, ref, d_send, d_recv.at[at(k)], me, partner)

    def e_copy(k, core):
        ref = xs.at[at(k), core, 1 - x]
        return remote(ref, ref, e_send, e_recv.at[at(k)], me, partner)

    def y_copy(k):
        s = at(k)
        return remote(ys.at[s], yd.at[s], y_send, f_recv.at[s], me, partner)

    def z_copy(k):
        s = at(k)
        return remote(zs.at[s], zx.at[s], z_send, a_recv.at[s], me, across)

    def h_copy(k):
        s = at(k)
        return remote(ns.at[s], na.at[s], n_send, r_recv.at[s], peer(k), tp)

    x_copy = remote(away_part, far_part, h_send, h_recv, me, across)

    def home(k):
        s = at(k)
        y_copy(k).wait_recv()
        for i in (1, 0):
            result = (own_y[s, i] + yd[s, i].astype(F32)).astype(BF)
            if k == own:
                na[0, i] = result
            else:
                ns[s, i] = result
        if k != own:
            h_copy(k).start()

    def r_copy(k):
        s = there(k)
        return remote(rs.at[at(k)], ra.at[s], r_send, r_recv.at[s], peer(k), tp)

    def r_arrival(k):
        s = at(k)
        return remote(rs.at[s], ra.at[s], r_send, r_recv.at[s], peer(k), tp)

    def take(k):
        if k != own:
            a_arrival(k).wait_recv()
            f_copy(k).start()
        d_copy(k, c).start()

    def pass_on(k):
        f_arrival(k).wait_recv()
        e_copy(k, c).start()

    def ready(k):
        d_copy(k, 1 - c).wait_recv()
        e_copy(k, 1 - c).wait_recv()

    def pair(k):
        s = at(k)
        y_copy(k).wait_recv()
        zs[s] = (own_y[s, 1] + yd[s, 1].astype(F32)).astype(BF)
        z_copy(k).start()
        za[s] = own_y[s, 0] + yd[s, 0].astype(F32)

    def give(k):
        s = at(k)
        z_copy(k).wait_recv()
        rs[s] = (za[s] + zx[s].astype(F32)).astype(BF)
        r_copy(k).start()

    ff = wg.shape[1]
    tile = 256 if ff % 256 == 0 else 128

    def normalize(k):
        s = at(k)
        pieces = [xs[s, q % CORES, q // CORES].astype(F32) for q in range(n_tp)]
        lanes = None
        for piece in pieces:
            square = piece * piece
            for j in range(0, width, 128):
                part = square[:, j:j + 128]
                lanes = part if lanes is None else lanes + part
        total = jnp.sum(lanes, axis=1, keepdims=True)
        factor = lax.rsqrt(total / (width * n_tp) + EPS)
        for q, piece in enumerate(pieces):
            block[:, q * width:(q + 1) * width] = (
                piece * factor * gains[q]
            ).astype(BF)

    def up_gate(k, part):
        for f in range(part * ff // 4, (part + 1) * ff // 4, tile):
            gate = jnp.dot(block[...], wg[:, f:f + tile], preferred_element_type=F32)
            up = jnp.dot(block[...], wu[:, f:f + tile], preferred_element_type=F32)
            hid[:, f:f + tile] = (gate / (1.0 + jnp.exp(-gate)) * up).astype(BF)

    def down_away(k):
        s = at(k)
        for i, q_x in ((1, 1 - x), (0, x)):
            ys[s, i] = jnp.dot(
                hid[...], wd[q_x * CORES + 1 - c], preferred_element_type=F32
            ).astype(BF)
        y_copy(k).start()

    def down_here(k):
        s = at(k)
        for i, q_x in ((1, 1 - x), (0, x)):
            own_y[s, i] = jnp.dot(hid[...], wd[q_x * CORES + c], preferred_element_type=F32)

    def mixed(k, back):
        return jnp.dot(mix_hi[at(k)], back, preferred_element_type=F32) + jnp.dot(
            mix_lo[at(k)], back, preferred_element_type=F32
        )

    def collect(k):
        h_copy(k).wait_recv()

    def swap(k):
        total = None
        for s in range(NEAR):
            part = mixed((s, s), na[s, 1])
            total = part if total is None else total + part
        away_part[...] = total.astype(BF)
        x_copy.start()

    def gather(k):
        total = None
        for s in range(NEAR):
            part = mixed((s, s), na[s, 0])
            total = part if total is None else total + part
        sums[...] = total

    def far_mix(k):
        r_arrival(k).wait_recv()
        sums[...] = sums[...] + mixed(k, ra[at(k)])

    with mark("gains"):
        for copy in g_arrivals:
            copy.wait_recv()

    def weights(k):
        for load in loads:
            load.wait()

    def only(where, action):
        def run(k):
            @pl.when(where)
            def _():
                action(k)
        return run

    places = {
        "<": outer == 1, ">": outer == 0, "{": outer + high == 2, "}": outer - high == 1,
        "[": outer - high == -1, "]": outer + high == 0,
    }
    todo = {
        "take": take, "pass": pass_on, "ready": ready, "norm": normalize, "load": weights,
        "away": down_away, "here": down_here, "pair": pair, "give": give,
        "home": home, "collect": collect, "swap": swap, "gather": gather, "mix": far_mix,
    }
    for part in range(4):
        todo["gu%d" % part] = functools.partial(up_gate, part=part)
    for word in ORDER:
        name, ks = word.split(":")
        k = slot_pair(ks)
        action = todo[name.strip("<>{}[]")]
        if name[0] in places:
            action = only(places[name[0]], action)
        with mark("%s_%s" % (name, ks.replace("/", "i"))):
            action(k)

    last = slot_pair(LAST)
    with mark("swapped"):
        x_copy.wait_recv()
    sums[...] = sums[...] + far_part[...].astype(F32)
    with mark("last"):
        r_arrival(last).wait_recv()
    out_ref[...] = (sums[...] + mixed(last, ra[at(last)])).astype(BF)

    with mark("sends"):
        mine, other = xs.at[:, c, x], xs.at[:, c, 1 - x]
        for ref, sem in (
            (send_a.at[pl.ds(1, n - 1)], a_send), (mine, f_send), (mine, d_send), (other, e_send),
            (ys, y_send), (zs.at[pl.ds(NEAR, n - NEAR)], z_send), (away_part, h_send),
            (rs.at[pl.ds(NEAR, n - NEAR)], r_send), (ns.at[pl.ds(1, NEAR - 1)], n_send),
            (gains.at[pl.ds(0, n_tp - 1)], g_send),
        ):
            remote(ref, ref, sem, h_recv, me, across).wait_send()


def slot_pair(word):
    parts = word.split("/")
    return int(parts[0]), int(parts[-1])


def routed(n, n_tp, tokens, norm_gain, expert_ids, gate_share, gate_weight, up_weight, down_weight):
    rows, width = tokens.shape
    experts = n * gate_weight.shape[0]
    cap = 4 * rows // experts
    depth, ff = gate_weight.shape[1:]
    hbm = pl.BlockSpec(memory_space=pltpu.HBM)
    dma = pltpu.SemaphoreType.DMA
    return pl.pallas_call(
        functools.partial(fused, n, n_tp),
        out_shape=pltpu.VMEM((rows, width), BF),
        in_specs=[hbm] * 7,
        out_specs=pl.BlockSpec(memory_space=pltpu.VMEM),
        scratch_shapes=[
            pltpu.VMEM((rows, width), BF),
            pltpu.VMEM((width,), BF),
            pltpu.VMEM((2, rows), jnp.int32),
            pltpu.VMEM((2, rows), F32),
            pltpu.VMEM((depth, ff), BF),
            pltpu.VMEM((depth, ff), BF),
            pltpu.VMEM((n_tp, ff, width), BF),
            pltpu.VMEM((n_tp, 1, width), F32),
            pltpu.VMEM((experts, rows), F32),
            pltpu.VMEM((experts, rows), F32),
            pltpu.VMEM((n, cap, width), BF),
            pltpu.VMEM((n, CORES, n_tp // CORES, cap, width), BF),
            pltpu.VMEM((cap, depth), BF),
            pltpu.VMEM((cap, ff), BF),
            pltpu.VMEM((n, 2, cap, width), F32),
            pltpu.VMEM((n, 2, cap, width), BF),
            pltpu.VMEM((n, 2, cap, width), BF),
            pltpu.VMEM((n, cap, width), F32),
            pltpu.VMEM((n, cap, width), BF),
            pltpu.VMEM((n, cap, width), BF),
            pltpu.VMEM((n, cap, width), BF),
            pltpu.VMEM((n, cap, width), BF),
            pltpu.VMEM((n // 2, 2, cap, width), BF),
            pltpu.VMEM((n // 2, 2, cap, width), BF),
            pltpu.VMEM((rows, width), BF),
            pltpu.VMEM((rows, width), BF),
            pltpu.VMEM((rows, width), F32),
            pltpu.VMEM((n, rows, cap), BF),
            pltpu.VMEM((n, rows, cap), BF),
            dma((4,)), dma((2 + n_tp,)),
            dma, dma((3,)),
            dma, dma((n,)),
            dma, dma((n,)),
            dma, dma((n,)),
            dma, dma((n,)),
            dma,
            dma,
            dma, dma((n,)),
            dma, dma, dma,
        ],
        compiler_params=pltpu.CompilerParams(
            collective_id=0, has_side_effects=True, vmem_limit_bytes=56 * 1024 * 1024
        ),
    )(
        tokens, norm_gain, expert_ids.T, gate_share.T,
        gate_weight, up_weight, down_weight,
    )


def shards(n, n_tp, *args):
    tokens, gate_weight = args[0], args[4]
    rows, width = tokens.shape
    cap = 4 * rows // (n * gate_weight.shape[0])
    fits = (
        n_tp == 2 * CORES and n == 4 * LINE and gate_weight.shape[0] == 1 and rows % 128 == 0
        and width % 128 == 0 and gate_weight.shape[2] % 128 == 0 and cap % 128 == 0
    )
    return routed(n, n_tp, *args) if fits else plain(*args)


def solution(mesh):
    body = functools.partial(shards, mesh.shape["ep"], mesh.shape["tp"])
    in_specs = (
        P("ep", "tp"),
        P("tp"),
        P("ep", None),
        P("ep", None),
        P("ep", None, "tp"),
        P("ep", None, "tp"),
        P("ep", "tp", None),
    )
    out_specs = P("ep", "tp")
    return jax.shard_map(body, mesh=mesh, in_specs=in_specs, out_specs=out_specs, check_vma=False)
```
